32 devices in a mesh: grp: 2 (over y), sp: 8 (over z, core), tp: 2 (over x).
Axes of the slice: x: 2, y: 2, z: 4, core: 2. Of those that a mesh axis runs over, the one named last changes fastest.
Arguments:
- queries: bfloat16 [12288, 1024], P(('grp', 'sp'), 'tp'), parts along dimension 0, may hold values from -200 to 200
- key_rows: bfloat16 [12288, 512], P(('grp', 'sp'), 'tp'), parts along dimension 0, may hold values from -6 to 6
- value_rows: bfloat16 [12288, 512], P(('grp', 'sp'), 'tp'), parts along dimension 0, may hold values from -6 to 6
- doc_ids: int32 [12288], P(('grp', 'sp')), parts along dimension 0, may hold values from 0 to 3, never falling along the last dimension, each value on 1 to 3072 neighbouring positions
- sink_logits: float32 [16], P('tp'), may hold values from 2 to 7
- out_weight: bfloat16 [1024, 2048], P('tp', 'sp'), may hold values from -0.1875 to 0.1875
- residual: bfloat16 [12288, 2048], P(('grp', 'sp', 'tp')), parts along dimension 0, may hold values from -6 to 6
- gain_mixed: float32 [2048], replicated, may hold values from 0.1 to 1.9
- gain_before: float32 [2048], replicated, may hold values from 0.1 to 1.9
- gain_after: float32 [2048], replicated, may hold values from 0.1 to 1.9
- gate_weight: bfloat16 [2048, 6144], P('sp', 'tp'), may hold values from -0.125 to 0.125
- up_weight: bfloat16 [2048, 6144], P('sp', 'tp'), may hold values from -0.125 to 0.125
- down_weight: bfloat16 [6144, 2048], P('tp', 'sp'), may hold values from -0.078125 to 0.078125
Outputs:
- layer_out: bfloat16 [12288, 2048], P(('grp', 'sp', 'tp')), parts along dimension 0
The draws below stay inside these ranges and needn't reach their ends.
There are 2 independent parts, one for each index of `grp`. The reference program is written for one: setup_inputs(seed, part) draws one part's arguments, and reference() takes and returns one part's arrays. A program takes and returns all parts, laid end to end along the dimension named above; an argument that names none is the same for every part. Nothing has to cross between parts.
All inputs are finite; a program needn't handle non-finite values.
Results may differ from the reference program's by a relative error of at most 0.015.
Values may be sent and summed in bfloat16 or wider, within the bound.
No kernel may reach another device: no remote copies, remote signals or barrier semaphores. Data moves between devices by JAX's collectives and lax.ppermute only.
A program may use at most 128 MiB of HBM per device.

```python
import math
import jax
import jax.numpy as jnp
import numpy as np
from jax import lax

D = 2048
HEADS = 16
KV_HEADS = 8
HEAD_DIM = 64
FF = 6144
WINDOW = 128
TOKENS = 6144
DOCS = 4
DOC_MOST = 3072
N_TP = 2


def drawn(key):
    base_keys = jnp.clip(jax.random.normal(jax.random.fold_in(key, 11), (TOKENS, KV_HEADS * HEAD_DIM), jnp.float32), -5.0, 5.0)
    base_queries = jnp.clip(jax.random.normal(jax.random.fold_in(key, 12), (TOKENS, HEADS * HEAD_DIM), jnp.float32), -5.0, 5.0)
    return (base_queries, base_keys)


def draw_queries(key, part):
    return drawn(key)[0].astype(jnp.bfloat16)


def draw_key_rows(key, part):
    return drawn(key)[1].astype(jnp.bfloat16)


def shard_levels(key, dims, pieces, smallest, top_value):
    level, own = 1.0, jax.random.fold_in(key, 6)
    for axis_at, blocks in pieces:
        heights = jnp.exp(jax.random.uniform(jax.random.fold_in(own, axis_at), (blocks,), jnp.float32, smallest / len(pieces), top_value / len(pieces)))
        level = level * jnp.repeat(heights, dims[axis_at] // blocks).reshape([-1 if axis == axis_at else 1 for axis in range(len(dims))])
    return level


def length_profile(amount, total, bound, skew):
    weights = [(1 << 20) // math.isqrt(rank ** skew) + 1 for rank in range(2, amount + 1)]
    spare, holding = total - bound - (amount - 1), [1] * (amount - 1)
    while spare > 0:
        candidates = [i for i in range(amount - 1) if holding[i] < bound]
        mass, remaining = sum([weights[i] for i in candidates]), spare
        for i in candidates:
            more = min(bound - holding[i], max(1, remaining * weights[i] // mass), spare)
            holding[i] = holding[i] + more
            spare = spare - more
    return np.array([bound] + holding)


def uneven_parts(stream_key, count, total, bound, skew):
    if count == 2:
        one = jax.random.randint(stream_key, (), max(1, total - bound), min(bound, total - 1) + 1)
        return jnp.stack([one, total - one])
    lengths = jnp.asarray(length_profile(count, total, bound, skew), jnp.int32)
    twos = (count - 1) // 2
    source_of, taker = lengths[1:1 + 2 * twos:2], lengths[2:2 + 2 * twos:2]
    margin = jnp.minimum(source_of - 1, bound - taker)
    moved = jax.random.randint(jax.random.fold_in(stream_key, 1), (twos,), 0, 1 << 20) % (margin + 1)
    lengths = lengths.at[1:1 + 2 * twos:2].set(source_of - moved).at[2:2 + 2 * twos:2].set(taker + moved)
    return lengths[jax.random.permutation(jax.random.fold_in(stream_key, 2), count)]


def centred(stream_key, dims, width, most, split=(), kind=jnp.bfloat16):
    level = shard_levels(stream_key, dims, split, -0.22, 0.18) if split else 1.0
    drawn = jax.random.normal(stream_key, dims, jnp.float32) * width * level
    return jnp.minimum(jnp.maximum(drawn, -most), most).astype(kind)


def setup_inputs(seed: int = 0, part: int = 0) -> dict:
    arg_keys = jax.random.split(jax.random.key(seed), 14)
    own_keys = jax.random.split(jax.random.fold_in(arg_keys[13], part), 14)
    return {
        "queries": draw_queries(jax.random.fold_in(jax.random.fold_in(arg_keys[13], part), 71), part),
        "key_rows": draw_key_rows(jax.random.fold_in(jax.random.fold_in(arg_keys[13], part), 71), part),
        "value_rows": centred(own_keys[2], (TOKENS, KV_HEADS * HEAD_DIM), 1.0, 6.0, ((0, 8), (1, 2))),
        "doc_ids": jnp.searchsorted(jnp.cumsum(uneven_parts(own_keys[3], DOCS, TOKENS, DOC_MOST, 1)), jnp.arange(TOKENS), side="right").astype(jnp.int32),
        "sink_logits": jnp.clip(2.0 + 5.0 * jax.random.uniform(arg_keys[4], (HEADS,), jnp.float32) ** shard_levels(arg_keys[4], (HEADS,), ((0, 2),), -0.2, 0.2), 2.0, 7.0),
        "out_weight": centred(arg_keys[5], (HEADS * HEAD_DIM, D), (HEADS * HEAD_DIM) ** -0.5, 0.1875, ((0, 2), (1, 8))),
        "residual": centred(own_keys[6], (TOKENS, D), 1.0, 6.0, ((0, 16),)),
        "gain_mixed": jnp.clip(1.0 + 0.18 * jax.random.normal(arg_keys[7], (D,), jnp.float32), 0.1, 1.9),
        "gain_before": jnp.clip(1.0 + 0.18 * jax.random.normal(arg_keys[8], (D,), jnp.float32), 0.1, 1.9),
        "gain_after": jnp.clip(1.0 + 0.18 * jax.random.normal(arg_keys[9], (D,), jnp.float32), 0.1, 1.9),
        "gate_weight": centred(arg_keys[10], (D, FF), D ** -0.5, 0.125, ((0, 8), (1, 2))),
        "up_weight": centred(arg_keys[11], (D, FF), D ** -0.5, 0.125, ((0, 8), (1, 2))),
        "down_weight": centred(arg_keys[12], (FF, D), FF ** -0.5, 0.078125, ((0, 2), (1, 8))),
    }


epsilon = 1e-06
masked_value = -1e+30

def stored(value):
    return lax.optimization_barrier(value.astype(jnp.bfloat16)).astype(jnp.float32)

def rms_scaled(value, gain):
    return value * lax.rsqrt(lax.optimization_barrier(jnp.mean(value * value, axis=-1, keepdims=True)) + epsilon) * gain

def reference(queries, key_rows, value_rows, doc_ids, sink_logits, out_weight, residual, gain_mixed, gain_before, gain_after, gate_weight, up_weight, down_weight):
    total = queries.shape[0]
    blocks = total // WINDOW
    group_size = HEADS // KV_HEADS
    padded_keys = jnp.concatenate([jnp.zeros((WINDOW, KV_HEADS * HEAD_DIM), jnp.bfloat16), key_rows], axis=0)
    padded_values = jnp.concatenate([jnp.zeros((WINDOW, KV_HEADS * HEAD_DIM), jnp.bfloat16), value_rows], axis=0)
    padded_docs = jnp.concatenate([jnp.zeros((WINDOW,), jnp.int32) - 1, doc_ids], axis=0)
    key_pos = jnp.arange(total + WINDOW, dtype=jnp.int32) - WINDOW

    def windows(array):
        first = array[:-WINDOW].reshape((blocks, WINDOW) + array.shape[1:])
        second = array[WINDOW:].reshape((blocks, WINDOW) + array.shape[1:])
        return jnp.concatenate([first, second], axis=1)
    key_blocks = windows(padded_keys).reshape(blocks, 2 * WINDOW, KV_HEADS, HEAD_DIM).astype(jnp.float32)
    value_blocks = windows(padded_values).reshape(blocks, 2 * WINDOW, KV_HEADS, HEAD_DIM).astype(jnp.float32)
    key_docs = windows(padded_docs)
    key_places = windows(key_pos)
    query_blocks = queries.reshape(blocks, WINDOW, KV_HEADS, group_size, HEAD_DIM).astype(jnp.float32)
    query_places = jnp.arange(total, dtype=jnp.int32).reshape(blocks, WINDOW)
    query_docs = doc_ids.reshape(blocks, WINDOW)
    scores = jnp.einsum('bqhgd,bkhd->bhgqk', query_blocks, key_blocks) * HEAD_DIM ** (-0.5)
    distance = query_places[:, :, None] - key_places[:, None, :]
    valid = (distance >= 0) & (distance < WINDOW) & (key_places[:, None, :] >= 0)
    valid = valid & (query_docs[:, :, None] == key_docs[:, None, :])
    scores = jnp.where(valid[:, None, None], scores, masked_value)
    sinks = sink_logits.reshape(KV_HEADS, group_size)[None, :, :, None]
    top = jnp.maximum(lax.optimization_barrier(jnp.max(scores, axis=-1)), sinks)
    weight = jnp.exp(scores - top[..., None])
    denom = lax.optimization_barrier(jnp.sum(weight, axis=-1)) + jnp.exp(sinks - top)
    weight_b = weight.astype(jnp.bfloat16).astype(jnp.float32)
    summed = jnp.einsum('bhgqk,bkhd->bqhgd', weight_b, value_blocks)
    scale = jnp.transpose(denom, (0, 3, 1, 2))[..., None]
    mixed = (summed / scale).reshape(total, HEADS * HEAD_DIM).astype(jnp.bfloat16)
    projected = stored(jnp.dot(mixed, out_weight, preferred_element_type=jnp.float32))
    after = stored(residual.astype(jnp.float32) + rms_scaled(projected, gain_mixed))
    normed = rms_scaled(after, gain_before).astype(jnp.bfloat16)
    gate = jnp.dot(normed, gate_weight, preferred_element_type=jnp.float32)
    upward = jnp.dot(normed, up_weight, preferred_element_type=jnp.float32)
    hidden = (jax.nn.silu(gate) * upward).astype(jnp.bfloat16)
    block_size = FF // N_TP
    summed_out = jnp.zeros((total, D), jnp.float32)
    for index in range(N_TP):
        partial_sum = jnp.dot(hidden[:, index * block_size:(index + 1) * block_size], down_weight[index * block_size:(index + 1) * block_size], preferred_element_type=jnp.float32)
        summed_out = summed_out + stored(partial_sum)
    ffn_out = stored(summed_out)
    return (after + 0.5 * rms_scaled(ffn_out, gain_after)).astype(jnp.bfloat16)
```

```python
import jax
import jax.numpy as jnp
from jax import lax
from jax.sharding import PartitionSpec as P

HEAD_DIM = 64
WINDOW = 128


epsilon = 1e-06
masked_value = -1e30


def passed_along(value, axis, steps):
    count = lax.axis_size(axis)
    first, last = (max(0, -steps), min(count, count - steps))
    return lax.ppermute(value, axis, [(source, source + steps) for source in range(first, last)])


def stored(value):
    return lax.optimization_barrier(value.astype(jnp.bfloat16)).astype(jnp.float32)


def rms_scaled(value, gain):
    return value * lax.rsqrt(jnp.mean(value * value, axis=-1, keepdims=True) + epsilon) * gain


def windows(array, blocks):
    first = array[:-WINDOW].reshape((blocks, WINDOW) + array.shape[1:])
    second = array[WINDOW:].reshape((blocks, WINDOW) + array.shape[1:])
    return jnp.concatenate([first, second], axis=1)


def attend(queries, key_rows, value_rows, doc_ids, sink_logits):
    length = queries.shape[0]
    blocks = length // WINDOW
    local_kv = key_rows.shape[1] // HEAD_DIM
    group_size = queries.shape[1] // HEAD_DIM // local_kv
    offset = lax.axis_index("sp") * length
    tail_keys, tail_values, tail_docs = passed_along(
        (key_rows[length - WINDOW :], value_rows[length - WINDOW :], doc_ids[length - WINDOW :]),
        "sp",
        1,
    )
    key_blocks = windows(jnp.concatenate([tail_keys, key_rows], axis=0), blocks).reshape(
        blocks, 2 * WINDOW, local_kv, HEAD_DIM
    )
    value_blocks = windows(jnp.concatenate([tail_values, value_rows], axis=0), blocks).reshape(
        blocks, 2 * WINDOW, local_kv, HEAD_DIM
    )
    key_docs = windows(jnp.concatenate([tail_docs, doc_ids], axis=0), blocks)
    key_places = windows(offset - WINDOW + jnp.arange(length + WINDOW, dtype=jnp.int32), blocks)
    query_places = (offset + jnp.arange(length, dtype=jnp.int32)).reshape(blocks, WINDOW)
    query_docs = doc_ids.reshape(blocks, WINDOW)
    query_blocks = queries.reshape(blocks, WINDOW, local_kv, group_size, HEAD_DIM)
    scores = jnp.einsum(
        "bqhgd,bkhd->bhgqk", query_blocks, key_blocks, preferred_element_type=jnp.float32
    ) * HEAD_DIM ** (-0.5)
    distance = query_places[:, :, None] - key_places[:, None, :]
    valid = (distance >= 0) & (distance < WINDOW) & (key_places[:, None, :] >= 0)
    valid = valid & (query_docs[:, :, None] == key_docs[:, None, :])
    scores = jnp.where(valid[:, None, None], scores, masked_value)
    sinks = sink_logits.reshape(local_kv, group_size)[None, :, :, None]
    top = jnp.maximum(jnp.max(scores, axis=-1), sinks)
    weight = jnp.exp(scores - top[..., None])
    denom = jnp.sum(weight, axis=-1) + jnp.exp(sinks - top)
    summed = jnp.einsum(
        "bhgqk,bkhd->bqhgd",
        weight.astype(jnp.bfloat16),
        value_blocks,
        preferred_element_type=jnp.float32,
    )
    scale = jnp.transpose(denom, (0, 3, 1, 2))[..., None]
    return (summed / scale).reshape(length, queries.shape[1]).astype(jnp.bfloat16)


def per_device(
    queries,
    key_rows,
    value_rows,
    doc_ids,
    sink_logits,
    out_weight,
    residual,
    gain_mixed,
    gain_before,
    gain_after,
    gate_weight,
    up_weight,
    down_weight,
):
    mixed = attend(queries, key_rows, value_rows, doc_ids, sink_logits)
    head_columns = lax.all_gather(out_weight, "sp", axis=1, tiled=True)
    projected = lax.psum_scatter(
        jnp.dot(mixed, head_columns, preferred_element_type=jnp.float32).astype(jnp.bfloat16),
        "tp",
        scatter_dimension=0,
        tiled=True,
    ).astype(jnp.float32)
    projected = stored(projected)
    after = stored(residual.astype(jnp.float32) + rms_scaled(projected, gain_mixed))
    normed = rms_scaled(after, gain_before).astype(jnp.bfloat16)
    full_gate, full_up, full_down = (
        lax.all_gather(gate_weight, "sp", axis=0, tiled=True),
        lax.all_gather(up_weight, "sp", axis=0, tiled=True),
        lax.all_gather(down_weight, "sp", axis=1, tiled=True),
    )
    piece = lax.all_gather(normed, "tp", axis=0, tiled=True)
    gate = jnp.dot(piece, full_gate, preferred_element_type=jnp.float32)
    upward = jnp.dot(piece, full_up, preferred_element_type=jnp.float32)
    hidden = (jax.nn.silu(gate) * upward).astype(jnp.bfloat16)
    ffn_out = stored(
        lax.psum_scatter(
            jnp.dot(hidden, full_down, preferred_element_type=jnp.float32).astype(jnp.bfloat16),
            "tp",
            scatter_dimension=0,
            tiled=True,
        ).astype(jnp.float32)
    )
    return (after + 0.5 * rms_scaled(ffn_out, gain_after)).astype(jnp.bfloat16)


def swapped(value, axis):
    return lax.ppermute(value, axis, [(0, 1), (1, 0)])


def gathered(shard, axis):
    count = lax.axis_size("sp")
    strided = [list(range(first, count, 2)) for first in range(2)]
    paired = [[first, first + 1] for first in range(0, count, 2)]
    part = lax.all_gather(shard, "sp", axis=axis, tiled=True, axis_index_groups=strided)
    return lax.all_gather(part, "sp", axis=axis, tiled=True, axis_index_groups=paired)


def columns_parted(value, count):
    width = value.shape[-1] // count
    pieces = value.reshape(value.shape[:-1] + (count // 2, 2, width))
    return jnp.swapaxes(pieces, -3, -2).reshape(value.shape)


def columns_joined(value, count):
    width = value.shape[-1] // count
    pieces = value.reshape(value.shape[:-1] + (2, count // 2, width))
    return jnp.swapaxes(pieces, -3, -2).reshape(value.shape)


def per_device_four(
    queries,
    key_rows,
    value_rows,
    doc_ids,
    sink_logits,
    out_weight,
    residual,
    gain_mixed,
    gain_before,
    gain_after,
    gate_weight,
    up_weight,
    down_weight,
):
    count = lax.axis_size("sp")
    units = gate_weight.shape[1] // 2
    first_unit = lax.axis_index("grp") * units
    rows = residual.shape[0]
    half = rows // 2

    both_out = jnp.concatenate([out_weight, swapped(out_weight, "tp")], axis=0)
    head_columns = gathered(both_out, 1)
    full_gate = gathered(lax.dynamic_slice_in_dim(gate_weight, first_unit, units, 1), 0)
    full_up = gathered(lax.dynamic_slice_in_dim(up_weight, first_unit, units, 1), 0)
    full_down = gathered(lax.dynamic_slice_in_dim(down_weight, first_unit, units, 0), 1)

    mixed = attend(queries, key_rows, value_rows, doc_ids, sink_logits)
    mine = lax.axis_index("tp") * rows
    received = swapped(lax.dynamic_slice_in_dim(mixed, rows - mine, rows, 0), "tp")
    kept = lax.dynamic_slice_in_dim(mixed, mine, rows, 0)
    projected = stored(
        jnp.dot(
            jnp.concatenate([kept, received], axis=1),
            head_columns,
            preferred_element_type=jnp.float32,
        )
    )
    parted_residual = columns_parted(residual, count).astype(jnp.float32)
    after = stored(parted_residual + rms_scaled(projected, columns_parted(gain_mixed, count)))
    normed = rms_scaled(after, columns_parted(gain_before, count)).astype(jnp.bfloat16)

    from_tp = swapped(normed, "tp")
    from_grp = swapped(normed, "grp")
    from_far = jnp.concatenate(
        [swapped(from_tp[:half], "grp"), swapped(from_grp[half:], "tp")], axis=0
    )

    def hidden_of(piece):
        gate = jnp.dot(piece, full_gate, preferred_element_type=jnp.float32)
        upward = jnp.dot(piece, full_up, preferred_element_type=jnp.float32)
        return (jax.nn.silu(gate) * upward).astype(jnp.bfloat16)

    def down_of(hidden):
        return jnp.dot(hidden, full_down, preferred_element_type=jnp.float32)

    hidden_near = hidden_of(jnp.concatenate([normed, from_tp], axis=0))
    hidden_far = hidden_of(jnp.concatenate([from_grp, from_far], axis=0))
    far = down_of(hidden_far[rows:]).astype(jnp.bfloat16)
    far_low = swapped(far[:half], "grp")
    far_high = swapped(far[half:], "tp")
    to_tp = down_of(hidden_near[rows:])
    to_tp = jnp.concatenate([to_tp[:half] + far_low.astype(jnp.float32), to_tp[half:]], axis=0)
    to_grp = down_of(hidden_far[:rows])
    to_grp = jnp.concatenate([to_grp[:half], to_grp[half:] + far_high.astype(jnp.float32)], axis=0)
    sent_tp = swapped(to_tp.astype(jnp.bfloat16), "tp")
    sent_grp = swapped(to_grp.astype(jnp.bfloat16), "grp")
    ffn_out = down_of(hidden_near[:rows])
    ffn_out = stored(ffn_out + sent_tp.astype(jnp.float32) + sent_grp.astype(jnp.float32))
    out = after + 0.5 * rms_scaled(ffn_out, columns_parted(gain_after, count))
    return columns_joined(out.astype(jnp.bfloat16), count)


def solution(mesh):
    shape = dict(mesh.shape)
    four = shape["grp"] == 2 and shape["tp"] == 2 and shape["sp"] % 2 == 0
    return jax.shard_map(
        per_device_four if four else per_device,
        mesh=mesh,
        in_specs=(
            P(("grp", "sp"), "tp"),
            P(("grp", "sp"), "tp"),
            P(("grp", "sp"), "tp"),
            P(("grp", "sp")),
            P("tp"),
            P("tp", "sp"),
            P(("grp", "sp", "tp"), None),
            P(),
            P(),
            P(),
            P("sp", "tp"),
            P("sp", "tp"),
            P("tp", "sp"),
        ),
        out_specs=P(("grp", "sp", "tp"), None),
        check_vma=False,
    )
```

```python
import jax
import jax.numpy as jnp
from jax import lax
from jax.experimental import pallas as pl
from jax.experimental.pallas import tpu as pltpu
from jax.sharding import PartitionSpec as P

HEAD_DIM = 64
WINDOW = 128


epsilon = 1e-06
masked_value = -1e30


def passed_along(value, axis, steps):
    count = lax.axis_size(axis)
    first, last = (max(0, -steps), min(count, count - steps))
    return lax.ppermute(value, axis, [(source, source + steps) for source in range(first, last)])


def stored(value):
    return lax.optimization_barrier(value.astype(jnp.bfloat16)).astype(jnp.float32)


def rms_scaled(value, gain):
    return value * lax.rsqrt(jnp.mean(value * value, axis=-1, keepdims=True) + epsilon) * gain


def windows(array, blocks):
    first = array[:-WINDOW].reshape((blocks, WINDOW) + array.shape[1:])
    second = array[WINDOW:].reshape((blocks, WINDOW) + array.shape[1:])
    return jnp.concatenate([first, second], axis=1)


def attend(queries, key_rows, value_rows, doc_ids, sink_logits):
    length = queries.shape[0]
    blocks = length // WINDOW
    local_kv = key_rows.shape[1] // HEAD_DIM
    group_size = queries.shape[1] // HEAD_DIM // local_kv
    offset = lax.axis_index("sp") * length
    tail_keys, tail_values, tail_docs = passed_along(
        (key_rows[length - WINDOW :], value_rows[length - WINDOW :], doc_ids[length - WINDOW :]),
        "sp",
        1,
    )
    key_blocks = windows(jnp.concatenate([tail_keys, key_rows], axis=0), blocks).reshape(
        blocks, 2 * WINDOW, local_kv, HEAD_DIM
    )
    value_blocks = windows(jnp.concatenate([tail_values, value_rows], axis=0), blocks).reshape(
        blocks, 2 * WINDOW, local_kv, HEAD_DIM
    )
    key_docs = windows(jnp.concatenate([tail_docs, doc_ids], axis=0), blocks)
    key_places = windows(offset - WINDOW + jnp.arange(length + WINDOW, dtype=jnp.int32), blocks)
    query_places = (offset + jnp.arange(length, dtype=jnp.int32)).reshape(blocks, WINDOW)
    query_docs = doc_ids.reshape(blocks, WINDOW)
    query_blocks = queries.reshape(blocks, WINDOW, local_kv, group_size, HEAD_DIM)
    scores = jnp.einsum(
        "bqhgd,bkhd->bhgqk", query_blocks, key_blocks, preferred_element_type=jnp.float32
    ) * HEAD_DIM ** (-0.5)
    distance = query_places[:, :, None] - key_places[:, None, :]
    valid = (distance >= 0) & (distance < WINDOW) & (key_places[:, None, :] >= 0)
    valid = valid & (query_docs[:, :, None] == key_docs[:, None, :])
    scores = jnp.where(valid[:, None, None], scores, masked_value)
    sinks = sink_logits.reshape(local_kv, group_size)[None, :, :, None]
    top = jnp.maximum(jnp.max(scores, axis=-1), sinks)
    weight = jnp.exp(scores - top[..., None])
    denom = jnp.sum(weight, axis=-1) + jnp.exp(sinks - top)
    summed = jnp.einsum(
        "bhgqk,bkhd->bqhgd",
        weight.astype(jnp.bfloat16),
        value_blocks,
        preferred_element_type=jnp.float32,
    )
    scale = jnp.transpose(denom, (0, 3, 1, 2))[..., None]
    return (summed / scale).reshape(length, queries.shape[1]).astype(jnp.bfloat16)


def per_device(
    queries,
    key_rows,
    value_rows,
    doc_ids,
    sink_logits,
    out_weight,
    residual,
    gain_mixed,
    gain_before,
    gain_after,
    gate_weight,
    up_weight,
    down_weight,
):
    mixed = attend(queries, key_rows, value_rows, doc_ids, sink_logits)
    head_columns = lax.all_gather(out_weight, "sp", axis=1, tiled=True)
    projected = lax.psum_scatter(
        jnp.dot(mixed, head_columns, preferred_element_type=jnp.float32).astype(jnp.bfloat16),
        "tp",
        scatter_dimension=0,
        tiled=True,
    ).astype(jnp.float32)
    projected = stored(projected)
    after = stored(residual.astype(jnp.float32) + rms_scaled(projected, gain_mixed))
    normed = rms_scaled(after, gain_before).astype(jnp.bfloat16)
    full_gate, full_up, full_down = (
        lax.all_gather(gate_weight, "sp", axis=0, tiled=True),
        lax.all_gather(up_weight, "sp", axis=0, tiled=True),
        lax.all_gather(down_weight, "sp", axis=1, tiled=True),
    )
    piece = lax.all_gather(normed, "tp", axis=0, tiled=True)
    gate = jnp.dot(piece, full_gate, preferred_element_type=jnp.float32)
    upward = jnp.dot(piece, full_up, preferred_element_type=jnp.float32)
    hidden = (jax.nn.silu(gate) * upward).astype(jnp.bfloat16)
    ffn_out = stored(
        lax.psum_scatter(
            jnp.dot(hidden, full_down, preferred_element_type=jnp.float32).astype(jnp.bfloat16),
            "tp",
            scatter_dimension=0,
            tiled=True,
        ).astype(jnp.float32)
    )
    return (after + 0.5 * rms_scaled(ffn_out, gain_after)).astype(jnp.bfloat16)


def swapped(value, axis):
    return lax.ppermute(value, axis, [(0, 1), (1, 0)])


def chip_permute(value, moves):
    pairs = [(2 * a + core, 2 * b + core) for a, b in moves for core in range(2)]
    return lax.ppermute(value, "sp", pairs)


def core_swapped(value):
    count = lax.axis_size("sp")
    return lax.ppermute(value, "sp", [(place, place ^ 1) for place in range(count)])


def chip_slots(shard):
    place = lax.axis_index("sp") // 2
    across = chip_permute(shard, [(0, 2), (1, 3), (2, 0), (3, 1)])
    upward = chip_permute(shard, [(0, 1), (1, 2), (2, 3)])
    downward = chip_permute(shard, [(1, 0), (2, 1), (3, 2)])
    carried = chip_permute(across, [(2, 3), (1, 0)])
    below = jnp.where(place == 0, carried, upward)
    above = jnp.where(place == 3, carried, downward)
    return [shard, across, below, above]


def slot_order():
    place = lax.axis_index("sp")
    chip, core = place // 2, place % 2
    chips = jnp.stack([chip, chip + 2, chip + 3, chip + 1]) % 4
    cores = jnp.stack([core, 1 - core])
    return (chips[:, None] * 2 + cores[None, :]).reshape(8).astype(jnp.int32)


def copy_body(order_ref, in_ref, out_ref):
    out_ref[...] = in_ref[...]


def reordered(value, order):
    rows, width = value.shape[0], value.shape[1] // order.shape[0]
    return pl.pallas_call(
        copy_body,
        grid_spec=pltpu.PrefetchScalarGridSpec(
            num_scalar_prefetch=1,
            grid=(order.shape[0],),
            in_specs=[pl.BlockSpec((rows, width), lambda i, order_ref: (0, order_ref[i]))],
            out_specs=pl.BlockSpec((rows, width), lambda i, order_ref: (0, i)),
        ),
        out_shape=jax.ShapeDtypeStruct(value.shape, value.dtype),
    )(order, value)


def gain_reordered(gain, order):
    return jnp.take(gain.reshape(order.shape[0], -1), order, axis=0).reshape(-1)


def per_device_four(
    queries,
    key_rows,
    value_rows,
    doc_ids,
    sink_logits,
    out_weight,
    residual,
    gain_mixed,
    gain_before,
    gain_after,
    gate_weight,
    up_weight,
    down_weight,
):
    order = slot_order()
    back = jnp.argsort(order).astype(jnp.int32)
    units = gate_weight.shape[1] // 2
    first_unit = lax.axis_index("grp") * units
    rows = residual.shape[0]
    half = rows // 2
    depth = gate_weight.shape[0]

    both_out = jnp.concatenate([out_weight, swapped(out_weight, "tp")], axis=0)
    out_slots = chip_slots(both_out)
    out_near = jnp.concatenate(out_slots, axis=1)
    out_far = core_swapped(out_near)
    width = both_out.shape[1]
    head_columns = jnp.concatenate(
        [
            piece
            for slot in range(4)
            for piece in (
                out_slots[slot],
                out_far[:, slot * width : (slot + 1) * width],
            )
        ],
        axis=1,
    )
    inner = chip_slots(
        jnp.concatenate(
            [
                lax.dynamic_slice_in_dim(gate_weight, first_unit, units, 1),
                lax.dynamic_slice_in_dim(up_weight, first_unit, units, 1),
            ],
            axis=0,
        )
    )
    outer = chip_slots(lax.dynamic_slice_in_dim(down_weight, first_unit, units, 0))
    inner = [piece for slot in inner for piece in (slot, core_swapped(slot))]
    full_gate = jnp.concatenate([piece[:depth] for piece in inner], axis=0)
    full_up = jnp.concatenate([piece[depth:] for piece in inner], axis=0)
    outer = [piece for slot in outer for piece in (slot, core_swapped(slot))]

    mixed = attend(queries, key_rows, value_rows, doc_ids, sink_logits)
    mine = lax.axis_index("tp") * rows
    received = swapped(lax.dynamic_slice_in_dim(mixed, rows - mine, rows, 0), "tp")
    kept = lax.dynamic_slice_in_dim(mixed, mine, rows, 0)
    projected = stored(
        jnp.dot(
            jnp.concatenate([kept, received], axis=1),
            head_columns,
            preferred_element_type=jnp.float32,
        )
    )
    moved_residual = reordered(residual, order).astype(jnp.float32)
    after = stored(moved_residual + rms_scaled(projected, gain_reordered(gain_mixed, order)))
    normed = rms_scaled(after, gain_reordered(gain_before, order)).astype(jnp.bfloat16)

    from_tp = swapped(normed, "tp")
    from_grp = swapped(normed, "grp")
    from_far = jnp.concatenate(
        [swapped(from_tp[:half], "grp"), swapped(from_grp[half:], "tp")], axis=0
    )

    def hidden_of(piece):
        gate = jnp.dot(piece, full_gate, preferred_element_type=jnp.float32)
        upward = jnp.dot(piece, full_up, preferred_element_type=jnp.float32)
        return (jax.nn.silu(gate) * upward).astype(jnp.bfloat16)

    hidden_near = hidden_of(jnp.concatenate([normed, from_tp], axis=0))
    hidden_far = hidden_of(jnp.concatenate([from_grp, from_far], axis=0))

    def summed_columns(full_down):
        def down_of(hidden):
            return jnp.dot(hidden, full_down, preferred_element_type=jnp.float32)

        far = down_of(hidden_far[rows:]).astype(jnp.bfloat16)
        far_low = swapped(far[:half], "grp").astype(jnp.float32)
        far_high = swapped(far[half:], "tp").astype(jnp.float32)
        to_tp = down_of(hidden_near[rows:])
        to_tp = jnp.concatenate([to_tp[:half] + far_low, to_tp[half:]], axis=0)
        to_grp = down_of(hidden_far[:rows])
        to_grp = jnp.concatenate([to_grp[:half], to_grp[half:] + far_high], axis=0)
        sent_tp = swapped(to_tp.astype(jnp.bfloat16), "tp")
        sent_grp = swapped(to_grp.astype(jnp.bfloat16), "grp")
        total = down_of(hidden_near[:rows])
        return total + sent_tp.astype(jnp.float32) + sent_grp.astype(jnp.float32)

    ffn_out = stored(
        jnp.concatenate(
            [
                summed_columns(jnp.concatenate(outer[:4], axis=1)),
                summed_columns(jnp.concatenate(outer[4:], axis=1)),
            ],
            axis=1,
        )
    )
    out = after + 0.5 * rms_scaled(ffn_out, gain_reordered(gain_after, order))
    return reordered(out.astype(jnp.bfloat16), back)


def solution(mesh):
    shape = dict(mesh.shape)
    four = shape["grp"] == 2 and shape["tp"] == 2 and shape["sp"] == 8
    return jax.shard_map(
        per_device_four if four else per_device,
        mesh=mesh,
        in_specs=(
            P(("grp", "sp"), "tp"),
            P(("grp", "sp"), "tp"),
            P(("grp", "sp"), "tp"),
            P(("grp", "sp")),
            P("tp"),
            P("tp", "sp"),
            P(("grp", "sp", "tp"), None),
            P(),
            P(),
            P(),
            P("sp", "tp"),
            P("sp", "tp"),
            P("tp", "sp"),
        ),
        out_specs=P(("grp", "sp", "tp"), None),
        check_vma=False,
    )
```

```python
import jax
import jax.numpy as jnp
from jax import lax
from jax.experimental import pallas as pl
from jax.experimental.pallas import tpu as pltpu
from jax.sharding import PartitionSpec as P

HEAD_DIM = 64
WINDOW = 128


epsilon = 1e-06
masked_value = -1e30


def passed_along(value, axis, steps):
    count = lax.axis_size(axis)
    first, last = (max(0, -steps), min(count, count - steps))
    return lax.ppermute(value, axis, [(source, source + steps) for source in range(first, last)])


def stored(value):
    return lax.optimization_barrier(value.astype(jnp.bfloat16)).astype(jnp.float32)


def rms_scaled(value, gain):
    return value * lax.rsqrt(jnp.mean(value * value, axis=-1, keepdims=True) + epsilon) * gain


def windows(array, blocks):
    first = array[:-WINDOW].reshape((blocks, WINDOW) + array.shape[1:])
    second = array[WINDOW:].reshape((blocks, WINDOW) + array.shape[1:])
    return jnp.concatenate([first, second], axis=1)


def tails_of(key_rows, value_rows, doc_ids):
    length = key_rows.shape[0]
    return passed_along(
        (key_rows[length - WINDOW :], value_rows[length - WINDOW :], doc_ids[length - WINDOW :]),
        "sp",
        1,
    )


def attend(queries, key_rows, value_rows, doc_ids, sink_logits, tails):
    length = queries.shape[0]
    blocks = length // WINDOW
    local_kv = key_rows.shape[1] // HEAD_DIM
    group_size = queries.shape[1] // HEAD_DIM // local_kv
    offset = lax.axis_index("sp") * length
    tail_keys, tail_values, tail_docs = tails
    key_blocks = windows(jnp.concatenate([tail_keys, key_rows], axis=0), blocks).reshape(
        blocks, 2 * WINDOW, local_kv, HEAD_DIM
    )
    value_blocks = windows(jnp.concatenate([tail_values, value_rows], axis=0), blocks).reshape(
        blocks, 2 * WINDOW, local_kv, HEAD_DIM
    )
    key_docs = windows(jnp.concatenate([tail_docs, doc_ids], axis=0), blocks)
    key_places = windows(offset - WINDOW + jnp.arange(length + WINDOW, dtype=jnp.int32), blocks)
    query_places = (offset + jnp.arange(length, dtype=jnp.int32)).reshape(blocks, WINDOW)
    query_docs = doc_ids.reshape(blocks, WINDOW)
    query_blocks = queries.reshape(blocks, WINDOW, local_kv, group_size, HEAD_DIM)
    scores = jnp.einsum(
        "bqhgd,bkhd->bhgqk", query_blocks, key_blocks, preferred_element_type=jnp.float32
    ) * HEAD_DIM ** (-0.5)
    distance = query_places[:, :, None] - key_places[:, None, :]
    valid = (distance >= 0) & (distance < WINDOW) & (key_places[:, None, :] >= 0)
    valid = valid & (query_docs[:, :, None] == key_docs[:, None, :])
    scores = jnp.where(valid[:, None, None], scores, masked_value)
    sinks = sink_logits.reshape(local_kv, group_size)[None, :, :, None]
    top = jnp.maximum(jnp.max(scores, axis=-1), sinks)
    weight = jnp.exp(scores - top[..., None])
    denom = jnp.sum(weight, axis=-1) + jnp.exp(sinks - top)
    summed = jnp.einsum(
        "bhgqk,bkhd->bqhgd",
        weight.astype(jnp.bfloat16),
        value_blocks,
        preferred_element_type=jnp.float32,
    )
    scale = jnp.transpose(denom, (0, 3, 1, 2))[..., None]
    return (summed / scale).reshape(length, queries.shape[1]).astype(jnp.bfloat16)


def per_device(
    queries,
    key_rows,
    value_rows,
    doc_ids,
    sink_logits,
    out_weight,
    residual,
    gain_mixed,
    gain_before,
    gain_after,
    gate_weight,
    up_weight,
    down_weight,
):
    mixed = attend(
        queries, key_rows, value_rows, doc_ids, sink_logits,
        tails_of(key_rows, value_rows, doc_ids),
    )
    head_columns = lax.all_gather(out_weight, "sp", axis=1, tiled=True)
    projected = lax.psum_scatter(
        jnp.dot(mixed, head_columns, preferred_element_type=jnp.float32).astype(jnp.bfloat16),
        "tp",
        scatter_dimension=0,
        tiled=True,
    ).astype(jnp.float32)
    projected = stored(projected)
    after = stored(residual.astype(jnp.float32) + rms_scaled(projected, gain_mixed))
    normed = rms_scaled(after, gain_before).astype(jnp.bfloat16)
    full_gate, full_up, full_down = (
        lax.all_gather(gate_weight, "sp", axis=0, tiled=True),
        lax.all_gather(up_weight, "sp", axis=0, tiled=True),
        lax.all_gather(down_weight, "sp", axis=1, tiled=True),
    )
    piece = lax.all_gather(normed, "tp", axis=0, tiled=True)
    gate = jnp.dot(piece, full_gate, preferred_element_type=jnp.float32)
    upward = jnp.dot(piece, full_up, preferred_element_type=jnp.float32)
    hidden = (jax.nn.silu(gate) * upward).astype(jnp.bfloat16)
    ffn_out = stored(
        lax.psum_scatter(
            jnp.dot(hidden, full_down, preferred_element_type=jnp.float32).astype(jnp.bfloat16),
            "tp",
            scatter_dimension=0,
            tiled=True,
        ).astype(jnp.float32)
    )
    return (after + 0.5 * rms_scaled(ffn_out, gain_after)).astype(jnp.bfloat16)


def swapped(value, axis):
    return lax.ppermute(value, axis, [(0, 1), (1, 0)])


def chip_permute(value, moves):
    pairs = [(2 * a + core, 2 * b + core) for a, b in moves for core in range(2)]
    return lax.ppermute(value, "sp", pairs)


def core_swapped(value):
    count = lax.axis_size("sp")
    return lax.ppermute(value, "sp", [(place, place ^ 1) for place in range(count)])


def chip_slots(shard):
    place = lax.axis_index("sp") // 2
    across = chip_permute(shard, [(0, 2), (1, 3), (2, 0), (3, 1)])
    upward = chip_permute(shard, [(0, 1), (1, 2), (2, 3)])
    downward = chip_permute(shard, [(1, 0), (2, 1), (3, 2)])
    carried = chip_permute(across, [(2, 3), (1, 0)])
    below = jnp.where(place == 0, carried, upward)
    above = jnp.where(place == 3, carried, downward)
    return [shard, across, below, above], across


def slot_order():
    place = lax.axis_index("sp")
    chip, core = place // 2, place % 2
    chips = jnp.stack([chip, chip + 2, chip + 3, chip + 1]) % 4
    cores = jnp.stack([core, 1 - core])
    return (chips[:, None] * 2 + cores[None, :]).reshape(8).astype(jnp.int32)


def copy_body(order_ref, in_ref, out_ref):
    count = order_ref.shape[0]
    width = in_ref.shape[1] // count
    for slot in range(count):
        start = pl.multiple_of(order_ref[slot] * width, width)
        out_ref[:, slot * width : (slot + 1) * width] = in_ref[:, pl.ds(start, width)]


def reordered(value, order):
    steps = 4
    block = (value.shape[0] // steps, value.shape[1])
    return pl.pallas_call(
        copy_body,
        grid_spec=pltpu.PrefetchScalarGridSpec(
            num_scalar_prefetch=1,
            grid=(steps,),
            in_specs=[pl.BlockSpec(block, lambda i, order_ref: (i, 0))],
            out_specs=pl.BlockSpec(block, lambda i, order_ref: (i, 0)),
        ),
        out_shape=jax.ShapeDtypeStruct(value.shape, value.dtype),
    )(order, value)


def slot_places():
    place = lax.axis_index("sp")
    block = jnp.arange(8, dtype=jnp.int32)
    ahead = (block // 2 - place // 2) % 4
    slot = jnp.where(ahead == 0, 0, jnp.where(ahead == 1, 3, ahead - 1))
    return (slot * 2 + (block + place) % 2).astype(jnp.int32)


def gain_reordered(gain, order):
    return jnp.take(gain.reshape(order.shape[0], -1), order, axis=0).reshape(-1)


def per_device_four(
    queries,
    key_rows,
    value_rows,
    doc_ids,
    sink_logits,
    out_weight,
    residual,
    gain_mixed,
    gain_before,
    gain_after,
    gate_weight,
    up_weight,
    down_weight,
):
    order = slot_order()
    back = slot_places()
    units = gate_weight.shape[1] // 2
    first_unit = lax.axis_index("grp") * units
    rows = residual.shape[0]
    half = rows // 2
    depth = gate_weight.shape[0]

    tails = tails_of(key_rows, value_rows, doc_ids)
    both_out = jnp.concatenate([out_weight, swapped(out_weight, "tp")], axis=0)
    tails, both_out = lax.optimization_barrier((tails, both_out))
    out_slots, mark = chip_slots(both_out)
    out_near = jnp.concatenate(out_slots, axis=1)
    out_far = core_swapped(out_near)
    width = both_out.shape[1]
    head_columns = jnp.concatenate(
        [
            piece
            for slot in range(4)
            for piece in (
                out_slots[slot],
                out_far[:, slot * width : (slot + 1) * width],
            )
        ],
        axis=1,
    )
    inner = jnp.concatenate(
        [
            lax.dynamic_slice_in_dim(gate_weight, first_unit, units, 1),
            lax.dynamic_slice_in_dim(up_weight, first_unit, units, 1),
        ],
        axis=0,
    )
    inner, _ = lax.optimization_barrier((inner, mark))
    inner, mark = chip_slots(inner)
    inner = [piece for slot in inner for piece in (slot, core_swapped(slot))]
    full_gate = jnp.concatenate([piece[:depth] for piece in inner], axis=0)
    full_up = jnp.concatenate([piece[depth:] for piece in inner], axis=0)

    mixed = attend(queries, key_rows, value_rows, doc_ids, sink_logits, tails)
    mine = lax.axis_index("tp") * rows
    received = swapped(lax.dynamic_slice_in_dim(mixed, rows - mine, rows, 0), "tp")
    kept = lax.dynamic_slice_in_dim(mixed, mine, rows, 0)
    projected = stored(
        jnp.dot(
            jnp.concatenate([kept, received], axis=1),
            head_columns,
            preferred_element_type=jnp.float32,
        )
    )
    moved_residual = reordered(residual, order).astype(jnp.float32)
    after = stored(moved_residual + rms_scaled(projected, gain_reordered(gain_mixed, order)))
    normed = rms_scaled(after, gain_reordered(gain_before, order)).astype(jnp.bfloat16)

    outer = lax.dynamic_slice_in_dim(down_weight, first_unit, units, 0)
    outer, _, _ = lax.optimization_barrier((outer, mark, normed))
    outer, _ = chip_slots(outer)
    outer = [piece for slot in outer for piece in (slot, core_swapped(slot))]
    from_tp = swapped(normed, "tp")
    from_grp = swapped(normed, "grp")
    from_far = jnp.concatenate(
        [swapped(from_tp[:half], "grp"), swapped(from_grp[half:], "tp")], axis=0
    )

    def hidden_of(piece):
        gate = jnp.dot(piece, full_gate, preferred_element_type=jnp.float32)
        upward = jnp.dot(piece, full_up, preferred_element_type=jnp.float32)
        return (jax.nn.silu(gate) * upward).astype(jnp.bfloat16)

    hidden_near = hidden_of(jnp.concatenate([normed, from_tp], axis=0))
    hidden_far = hidden_of(jnp.concatenate([from_grp, from_far], axis=0))

    def summed_columns(full_down):
        def down_of(hidden):
            return jnp.dot(hidden, full_down, preferred_element_type=jnp.float32)

        far = down_of(hidden_far[rows:]).astype(jnp.bfloat16)
        far_low = swapped(far[:half], "grp").astype(jnp.float32)
        far_high = swapped(far[half:], "tp").astype(jnp.float32)
        to_tp = down_of(hidden_near[rows:])
        to_tp = jnp.concatenate([to_tp[:half] + far_low, to_tp[half:]], axis=0)
        to_grp = down_of(hidden_far[:rows])
        to_grp = jnp.concatenate([to_grp[:half], to_grp[half:] + far_high], axis=0)
        sent_tp = swapped(to_tp.astype(jnp.bfloat16), "tp")
        sent_grp = swapped(to_grp.astype(jnp.bfloat16), "grp")
        total = down_of(hidden_near[:rows])
        return total + sent_tp.astype(jnp.float32) + sent_grp.astype(jnp.float32)

    ffn_out = stored(
        jnp.concatenate(
            [
                summed_columns(jnp.concatenate(outer[:4], axis=1)),
                summed_columns(jnp.concatenate(outer[4:], axis=1)),
            ],
            axis=1,
        )
    )
    out = after + 0.5 * rms_scaled(ffn_out, gain_reordered(gain_after, order))
    return reordered(out.astype(jnp.bfloat16), back)


def solution(mesh):
    shape = dict(mesh.shape)
    four = shape["grp"] == 2 and shape["tp"] == 2 and shape["sp"] == 8
    return jax.shard_map(
        per_device_four if four else per_device,
        mesh=mesh,
        in_specs=(
            P(("grp", "sp"), "tp"),
            P(("grp", "sp"), "tp"),
            P(("grp", "sp"), "tp"),
            P(("grp", "sp")),
            P("tp"),
            P("tp", "sp"),
            P(("grp", "sp", "tp"), None),
            P(),
            P(),
            P(),
            P("sp", "tp"),
            P("sp", "tp"),
            P("tp", "sp"),
        ),
        out_specs=P(("grp", "sp", "tp"), None),
        check_vma=False,
    )
```
